32 devices in a mesh: grp: 2 (over y), sp: 4 (over z), tp: 4 (over x, core).
Axes of the slice: x: 2, y: 2, z: 4, core: 2. Of those that a mesh axis runs over, the one named last changes fastest.
Arguments:
- tokens: bfloat16 [4096, 2048], P(('grp', 'sp')), parts along dimension 0, may hold values from -6 to 6
- fresh_token_input: bfloat16 [4096], P('grp'), parts along dimension 0, may hold values from -6 to 6
- value_matrix: bfloat16 [2048, 2048], P(None, 'tp'), may hold values from -0.125 to 0.125
- write_matrix: bfloat16 [2048, 1024], P(None, 'tp'), may hold values from -0.125 to 0.125
- read_matrix: bfloat16 [2048, 1024], P(None, 'tp'), may hold values from -0.125 to 0.125
- gate_matrix: bfloat16 [2048, 2048], P(None, 'tp'), may hold values from -0.125 to 0.125
- step_matrix: bfloat16 [2048, 32], replicated, may hold values from -0.125 to 0.125
- value_filter_taps: bfloat16 [4, 2048], replicated, may hold values from -3 to 3
- write_filter_taps: bfloat16 [4, 1024], replicated, may hold values from -3 to 3
- read_filter_taps: bfloat16 [4, 1024], replicated, may hold values from -3 to 3
- head_log_decay: float32 [32], replicated
- step_offset_bias: float32 [32], replicated, may hold values from -3.5 to -2.5
- decay_spike: float32 [4096, 32], P(('grp', 'sp'), 'tp'), parts along dimension 0, may hold values from -3 to 0, as said below
- bypass_scale: float32 [32], replicated, may hold values from 0.5 to 2
- group_norm_scale: float32 [2048], replicated, may hold values from 0.1 to 1.9
Outputs:
- prompt_out: bfloat16 [4096, 2048], P(('grp', 'sp'), 'tp'), parts along dimension 0
- state_cache: bfloat16 [256, 2048], P(('grp', 'sp'), 'tp'), parts along dimension 0
- step_out: bfloat16 [1024, 4], P(('grp', 'tp'), 'sp'), parts along dimension 0
The draws below stay inside these ranges and needn't reach their ends.
There are 2 independent parts, one for each index of `grp`. The reference program is written for one: setup_inputs(seed, part) draws one part's arguments, and reference() takes and returns one part's arrays. A program takes and returns all parts, laid end to end along the dimension named above; an argument that names none is the same for every part. Nothing has to cross between parts.
Inputs may be any that keep to these rules, and one draw needn't show every extreme that they name: `decay_spike`: never positive.
All inputs are finite; a program needn't handle non-finite values.
Results may differ from the reference program's by a relative error of at most 0.023.
Values may be sent and summed in bfloat16 or wider, within the bound.
A program may use at most 64 MiB of HBM per device.

```python
import jax
import jax.numpy as jnp
from jax import lax

D = 2048
HEADS = 32
HEAD = 64
GROUPS = 8
STATE = 128
CONV = 4
BLOCK = 128
TOK_DEV = 512
INNER = 2048
TOKENS = 2048
N_SP = 4


def draw_head_log_decay(key, part):
    key_pick, key_fast, key_slow = jax.random.split(jax.random.fold_in(key, 11), 3)
    chance = 0.5
    fast_pick = jax.random.uniform(key_pick, (HEADS,), jnp.float32) < chance
    fast_rate = jax.random.uniform(key_fast, (HEADS,), jnp.float32, 0.3, 1.0)
    slow_rate = jnp.exp(jax.random.uniform(key_slow, (HEADS,), jnp.float32, jnp.log(5.0 / TOKENS), jnp.log(12.0 / TOKENS)))
    return jnp.log(jnp.where(fast_pick, fast_rate, slow_rate)).astype(jnp.float32)


def draw_decay_spike(key, part):
    key_span, key_place, key_drop = jax.random.split(jax.random.fold_in(key, 23), 3)
    span_count = TOKENS // TOK_DEV
    span_scale = jnp.exp(jax.random.uniform(key_span, (span_count, HEADS), jnp.float32, jnp.log(0.5), jnp.log(2.0)))
    baseline_tier = -0.3 / TOKENS * jnp.repeat(span_scale, TOK_DEV, axis=0)
    places = jax.random.randint(key_place, (3,), 0, TOKENS)
    omitted_occasions = jnp.log(jax.random.uniform(key_drop, (3, HEADS), jnp.float32, 0.5, 0.8))
    agreeing_tally = (jnp.arange(TOKENS)[:, None] == places[None, :]).astype(jnp.float32)
    sudden_surges = jnp.sum(agreeing_tally[:, :, None] * omitted_occasions[None], axis=1)
    return (baseline_tier + sudden_surges).astype(jnp.float32)


def level_of(stream_key, shape, shards, low, largest):
    loudness, own = 1.0, jax.random.fold_in(stream_key, 6)
    for dim, shards_of in shards:
        heights = jnp.exp(jax.random.uniform(jax.random.fold_in(own, dim), (shards_of,), jnp.float32, low / len(shards), largest / len(shards)))
        loudness = loudness * jnp.repeat(heights, shape[dim] // shards_of).reshape([-1 if axis == dim else 1 for axis in range(len(shape))])
    return loudness


def bell_draw(key, dims, scale, most, cuts=(), held_as=jnp.bfloat16):
    level = level_of(key, dims, cuts, -0.22, 0.18) if cuts else 1.0
    values = jax.random.normal(key, dims, jnp.float32) * scale * level
    return jnp.minimum(jnp.maximum(values, -most), most).astype(held_as)


def setup_inputs(seed: int = 0, part: int = 0) -> dict:
    arg_keys = jax.random.split(jax.random.key(seed), 16)
    part_splits = jax.random.split(jax.random.fold_in(arg_keys[15], part), 16)
    tokens = bell_draw(part_splits[0], (TOKENS, D), 1.0, 6.0, ((0, 4),))
    fresh_token_input = bell_draw(part_splits[1], (D,), 1.0, 6.0)
    value_matrix = bell_draw(arg_keys[2], (D, INNER), D ** -0.5, 0.125, ((1, 4),))
    write_matrix = bell_draw(arg_keys[3], (D, GROUPS * STATE), D ** -0.5, 0.125, ((1, 4),))
    read_matrix = bell_draw(arg_keys[4], (D, GROUPS * STATE), D ** -0.5, 0.125, ((1, 4),))
    gate_matrix = bell_draw(arg_keys[5], (D, INNER), D ** -0.5, 0.125, ((1, 4),))
    step_matrix = bell_draw(arg_keys[6], (D, HEADS), D ** -0.5, 0.125)
    value_filter_taps = bell_draw(arg_keys[7], (CONV, INNER), CONV ** -0.5, 3.0)
    write_filter_taps = bell_draw(arg_keys[8], (CONV, GROUPS * STATE), CONV ** -0.5, 3.0)
    read_filter_taps = bell_draw(arg_keys[9], (CONV, GROUPS * STATE), CONV ** -0.5, 3.0)
    head_log_decay = draw_head_log_decay(jax.random.fold_in(arg_keys[15], 71), part)
    step_offset_bias = jnp.clip(jax.random.uniform(arg_keys[11], (HEADS,), jnp.float32, -3.5, -2.5), -3.5, -2.5)
    decay_spike = draw_decay_spike(jax.random.fold_in(jax.random.fold_in(arg_keys[15], part), 71), part)
    bypass_scale = jnp.clip(jax.random.uniform(arg_keys[13], (HEADS,), jnp.float32, 0.5, 2.0), 0.5, 2.0)
    group_norm_scale = jnp.clip(1.0 + 0.18 * jax.random.normal(arg_keys[14], (INNER,), jnp.float32), 0.1, 1.9)
    return {"tokens": tokens, "fresh_token_input": fresh_token_input, "value_matrix": value_matrix, "write_matrix": write_matrix, "read_matrix": read_matrix, "gate_matrix": gate_matrix, "step_matrix": step_matrix, "value_filter_taps": value_filter_taps, "write_filter_taps": write_filter_taps, "read_filter_taps": read_filter_taps, "head_log_decay": head_log_decay, "step_offset_bias": step_offset_bias, "decay_spike": decay_spike, "bypass_scale": bypass_scale, "group_norm_scale": group_norm_scale}


epsilon = 1e-06

def project(operand, weights):
    return jnp.dot(operand, weights, preferred_element_type=jnp.float32).astype(jnp.bfloat16)

def apply_taps(previous, current, tap_weights):
    joined = jnp.concatenate([previous, current], axis=0).astype(jnp.float32)
    length = current.shape[0]
    summed = jnp.zeros(current.shape, jnp.float32)
    for offset in range(CONV):
        summed = summed + tap_weights[offset].astype(jnp.float32) * joined[offset:offset + length]
    return summed

def group_norm(gated_rows, groups):
    shaped = gated_rows.reshape(gated_rows.shape[:-1] + (groups, -1))
    normed = shaped * lax.rsqrt(lax.optimization_barrier(jnp.mean(shaped * shaped, axis=-1, keepdims=True)) + epsilon)
    return normed.reshape(gated_rows.shape)

def reference(tokens, fresh_token_input, value_matrix, write_matrix, read_matrix, gate_matrix, step_matrix, value_filter_taps, write_filter_taps, read_filter_taps, head_log_decay, step_offset_bias, decay_spike, bypass_scale, group_norm_scale):
    per_group = HEADS // GROUPS
    value_rows = project(tokens, value_matrix)
    write_rows = project(tokens, write_matrix)
    read_rows = project(tokens, read_matrix)
    gate_rows = project(tokens, gate_matrix)
    step_raw = jnp.dot(tokens, step_matrix, preferred_element_type=jnp.float32)
    zero_wide = jnp.zeros((CONV - 1, INNER), jnp.bfloat16)
    zero_maps = jnp.zeros((CONV - 1, GROUPS * STATE), jnp.bfloat16)
    values = jax.nn.silu(apply_taps(zero_wide, value_rows, value_filter_taps)).astype(jnp.bfloat16)
    writes = jax.nn.silu(apply_taps(zero_maps, write_rows, write_filter_taps)).astype(jnp.bfloat16)
    reads = jax.nn.silu(apply_taps(zero_maps, read_rows, read_filter_taps)).astype(jnp.bfloat16)
    step_length = jax.nn.softplus(step_raw + step_offset_bias)
    head_decay_rates = jnp.exp(head_log_decay)
    log_decay_value = decay_spike - step_length * head_decay_rates
    blocks = TOKENS // BLOCK
    block_values = values.reshape(blocks, BLOCK, GROUPS, per_group, HEAD)
    block_writes = writes.reshape(blocks, BLOCK, GROUPS, STATE)
    block_reads = reads.reshape(blocks, BLOCK, GROUPS, STATE)
    block_steps = step_length.reshape(blocks, BLOCK, GROUPS, per_group)
    segment_fading = log_decay_value.reshape(blocks, BLOCK, GROUPS, per_group)
    causal = jnp.tril(jnp.ones((BLOCK, BLOCK), bool))

    def block_step(entering, inputs):
        val_in, wri_in, rea_in, stp_in, dec_in = inputs
        cumulative = jnp.cumsum(dec_in, axis=0)
        scores = jnp.einsum('lgn,sgn->gls', rea_in.astype(jnp.float32), wri_in.astype(jnp.float32))
        cum_heads = jnp.transpose(cumulative, (1, 2, 0))
        decay_gaps = cum_heads[:, :, :, None] - cum_heads[:, :, None, :]
        step_heads = jnp.transpose(stp_in, (1, 2, 0))
        mixing = (scores[:, None] * jnp.exp(jnp.where(causal, decay_gaps, -jnp.inf)) * step_heads[:, :, None, :]).astype(jnp.bfloat16)
        inner_part = jnp.einsum('gels,sgep->lgep', mixing.astype(jnp.float32), val_in.astype(jnp.float32))
        block_end = cumulative[-1]
        scaled = ((jnp.exp(block_end[None] - cumulative) * stp_in)[..., None] * val_in.astype(jnp.float32)).astype(jnp.bfloat16)
        block_state = jnp.einsum('sgn,sgep->ngep', wri_in.astype(jnp.float32), scaled.astype(jnp.float32))
        carried = jnp.exp(cumulative)[..., None] * jnp.einsum('lgn,ngep->lgep', rea_in.astype(jnp.float32), entering, precision=lax.Precision.HIGHEST)
        leaving = jnp.exp(block_end)[None, :, :, None] * entering + block_state
        return (leaving, inner_part + carried)
    initial = jnp.zeros((STATE, GROUPS, per_group, HEAD), jnp.float32)
    final_state, outputs = lax.scan(block_step, initial, (block_values, block_writes, block_reads, block_steps, segment_fading))
    mixed_rows = outputs.reshape(TOKENS, HEADS, HEAD) + bypass_scale[None, :, None] * values.astype(jnp.float32).reshape(TOKENS, HEADS, HEAD)
    gated_rows = mixed_rows.reshape(TOKENS, INNER) * jax.nn.silu(gate_rows.astype(jnp.float32))
    prompt_out = (group_norm(gated_rows, GROUPS) * group_norm_scale).astype(jnp.bfloat16)
    state_cache = final_state.reshape(STATE, INNER).astype(jnp.bfloat16)
    new_row = fresh_token_input[None]
    new_value = project(new_row, value_matrix)
    new_write = project(new_row, write_matrix)
    new_read = project(new_row, read_matrix)
    new_gate = project(new_row, gate_matrix)
    new_step = jax.nn.softplus(jnp.dot(new_row, step_matrix, preferred_element_type=jnp.float32)[0] + step_offset_bias)
    edge = TOKENS - (CONV - 1)
    new_values = jax.nn.silu(apply_taps(value_rows[edge:], new_value, value_filter_taps)).astype(jnp.bfloat16)
    latest_stores = jax.nn.silu(apply_taps(write_rows[edge:], new_write, write_filter_taps)).astype(jnp.bfloat16)
    new_reads = jax.nn.silu(apply_taps(read_rows[edge:], new_read, read_filter_taps)).astype(jnp.bfloat16)
    value_now = new_values.astype(jnp.float32).reshape(GROUPS, per_group, HEAD)
    write_now = latest_stores.astype(jnp.float32).reshape(GROUPS, STATE)
    read_now = new_reads.astype(jnp.float32).reshape(GROUPS, STATE)
    new_decay = jnp.exp(-new_step * head_decay_rates).reshape(GROUPS, per_group)
    step_now = new_step.reshape(GROUPS, per_group)
    cached = state_cache.astype(jnp.float32).reshape(STATE, GROUPS, per_group, HEAD)
    updated = new_decay[None, :, :, None] * cached + step_now[None, :, :, None] * write_now.T[:, :, None, None] * value_now[None]
    reading = jnp.einsum('gn,ngep->gep', read_now, updated, precision=lax.Precision.HIGHEST)
    new_mixed = reading + bypass_scale.reshape(GROUPS, per_group)[:, :, None] * value_now
    new_gated = new_mixed.reshape(1, INNER) * jax.nn.silu(new_gate.astype(jnp.float32))
    step_out = (group_norm(new_gated, GROUPS) * group_norm_scale).astype(jnp.bfloat16)[0]
    step_out = step_out.reshape(INNER // N_SP, N_SP)
    return (prompt_out, state_cache, step_out)
```

```python
import functools

import jax
import jax.numpy as jnp
from jax import lax
from jax.experimental import pallas as pl
from jax.experimental.pallas import tpu as pltpu
from jax.sharding import PartitionSpec as P

HEAD = 64
STATE = 128
CONV = 4
BLOCK = 128
PAD = 16
LANES = 128
EPSILON = 1e-06
F32 = jnp.float32
BF16 = jnp.bfloat16
MESH = pl.DeviceIdType.MESH


def dot(a, b, dims=((1,), (0,)), precision=None):
    return lax.dot_general(a, b, (dims, ((), ())), precision=precision, preferred_element_type=F32)


def silu(x):
    half = 0.5 * x
    return half + half * jnp.tanh(half)


def softplus(x):
    return jnp.maximum(x, 0.0) + jnp.log1p(jnp.exp(-jnp.abs(x)))


def split(x):
    high = x.astype(BF16)
    return jnp.concatenate([high.astype(F32), x - high.astype(F32)], axis=0).astype(BF16)


def kernel(
    n, tokens, fresh, w_value, w_write, w_read, w_gate, step_t, taps_v, taps_w, taps_r,
    log_rate, offset_bias, spike_t, bypass, gain,
    out, cache_out, step_out,
    xs, wv, ww, wr, wg, pv, pw, pr, pg, raw_t, vals, wrt, rds, y_loc, fade, local_state,
    received, sending, cache, step_row, step_recv, result,
    load_sem, halo_send, halo_recv, chain_send, chain_recv, cache_send, cache_recv,
    row_send, row_recv, out_sem,
):
    rows, width = tokens.shape
    channels = w_value.shape[1]
    maps = w_write.shape[1]
    groups = maps // STATE
    heads = channels // HEAD
    per_group = heads // groups
    wide = per_group * HEAD
    blocks = rows // BLOCK
    all_heads = step_t.shape[0]
    piece = STATE // n
    tp = lax.axis_index("tp")
    me = lax.axis_index("sp")
    last = n - 1
    chunks = channels // LANES
    chunks_group = wide // LANES

    loads = []

    def load(src, dst):
        copy = pltpu.make_async_copy(src, dst, load_sem.at[len(loads)])
        loads.append(copy)
        copy.start()
        return copy

    get_tokens = load(tokens, xs.at[pl.ds(PAD, rows)])
    get_gate = [load(w_gate.at[:, pl.ds(g * wide, wide)], wg.at[:, pl.ds(g * wide, wide)]) for g in range(groups)]
    get_write = load(w_write, ww)
    get_value = [load(w_value.at[:, pl.ds(g * wide, wide)], wv.at[:, pl.ds(g * wide, wide)]) for g in range(groups)]
    get_read = load(w_read, wr)

    barrier = pltpu.get_barrier_semaphore()

    @pl.when(me > 0)
    def _():
        pl.semaphore_signal(barrier, inc=1, device_id={"sp": me - 1}, device_id_type=MESH)

    @pl.when(me < last)
    def _():
        pl.semaphore_wait(barrier, 1)

    following = jnp.minimum(me + 1, last)
    halo = pltpu.make_async_remote_copy(
        src_ref=tokens.at[pl.ds(rows - PAD, PAD)], dst_ref=xs.at[pl.ds(0, PAD)],
        send_sem=halo_send, recv_sem=halo_recv, device_id={"sp": following}, device_id_type=MESH,
    )

    @pl.when(me < last)
    def _():
        halo.start()

    fresh_f = fresh[...].astype(F32)
    fresh_row = jnp.concatenate([fresh_f[i : i + 1] for i in range(width // LANES)], axis=1)
    xs[pl.ds(PAD + rows, PAD)] = jnp.broadcast_to(fresh_row, (PAD, width)).astype(BF16)

    @pl.when(me == 0)
    def _():
        xs[pl.ds(0, PAD)] = jnp.zeros((PAD, width), BF16)

    lane = lax.broadcasted_iota(jnp.int32, (heads, all_heads), 1)
    own = lane == lax.broadcasted_iota(jnp.int32, (heads, all_heads), 0) + tp * heads

    def column(ref):
        return jnp.sum(jnp.where(own, ref[...], 0.0), axis=1, keepdims=True)

    rates = jnp.exp(column(log_rate))
    bias = column(offset_bias)
    expand = (
        lax.broadcasted_iota(jnp.int32, (heads, channels), 1) // HEAD
        == lax.broadcasted_iota(jnp.int32, (heads, channels), 0)
    ).astype(F32)
    expand2 = jnp.concatenate([expand, expand], axis=0).astype(BF16)

    def spread(x):
        return dot(split(x), expand2, ((0,), (0,)))

    skip_row = jnp.sum(expand * column(bypass), axis=0, keepdims=True)
    gain_row = jnp.concatenate(
        [gain[pl.ds(tp * (channels // LANES) + i, 1)] for i in range(channels // LANES)], axis=1
    )

    get_tokens.wait()
    raw = dot(xs[pl.ds(PAD, rows + PAD)], step_t[...], ((1,), (1,)))
    raw_t[...] = raw[:rows].T
    if heads % 8 == 0:
        own_raw = raw_t[pl.ds(pl.multiple_of(tp * heads, 8), heads)]
    else:
        own_raw = dot(own.astype(F32), raw_t[...], precision=lax.Precision.HIGHEST)
    raw_new = jnp.sum(jnp.where(own, raw[rows : rows + 1], 0.0), axis=1, keepdims=True)
    step = softplus(own_raw + bias)
    new_step = softplus(raw_new + bias)
    log_decay = spike_t[...] - step * rates
    upper = (
        lax.broadcasted_iota(jnp.int32, (BLOCK, BLOCK), 0)
        <= lax.broadcasted_iota(jnp.int32, (BLOCK, BLOCK), 1)
    ).astype(F32)
    cums = [
        dot(log_decay[:, k * BLOCK : (k + 1) * BLOCK], upper, precision=lax.Precision.HIGHEST)
        for k in range(blocks)
    ]
    ends = [c[:, BLOCK - 1 :] for c in cums]
    before = [jnp.zeros_like(ends[0])]
    for k in range(blocks):
        before.append(before[k] + ends[k])
    scale_in = jnp.concatenate([jnp.exp(ends[k] - cums[k]) for k in range(blocks)], axis=1) * step
    cum_cols = [c.T for c in cums]
    end_rows = [jnp.sum(expand * jnp.exp(e), axis=0, keepdims=True) for e in ends]
    total_row = jnp.sum(expand * jnp.exp(before[blocks]), axis=0, keepdims=True)

    for g in range(groups):
        cols = pl.ds(g * wide, wide)
        get_gate[g].wait()
        pg[:, cols] = dot(xs[pl.ds(PAD, rows + PAD)], wg[:, cols])

    @pl.when(me > 0)
    def _():
        halo.wait_recv()

    def conv(src, taps, base, cols, start, count):
        own_cols = pl.ds(pl.multiple_of(base + cols.start, LANES), cols.size)
        weights = taps[:, own_cols].astype(F32)
        total = None
        for k in range(CONV):
            term = weights[k : k + 1] * src[pl.ds(start - (CONV - 1) + k, count), cols]
            total = term if total is None else total + term
        return silu(total)

    get_write.wait()
    pw[...] = dot(xs[...], ww[...])
    for g in range(groups):
        cols = pl.ds(g * STATE, STATE)
        for k in range(blocks):
            wrt[pl.ds(k * BLOCK, BLOCK), cols] = conv(pw, taps_w, tp * maps, cols, PAD + k * BLOCK, BLOCK).astype(BF16)

    def chain(c):
        return pltpu.make_async_remote_copy(
            src_ref=sending.at[c], dst_ref=received.at[c], send_sem=chain_send.at[c],
            recv_sem=chain_recv.at[c], device_id={"sp": following}, device_id_type=MESH,
        )

    inside = [[None] * blocks for _ in range(groups)]
    for g in range(groups):
        cols = pl.ds(g * wide, wide)
        get_value[g].wait()
        pv[:, cols] = dot(xs[...], wv[:, cols])
        lo, hi = g * wide, (g + 1) * wide
        running = None
        for k in range(blocks):
            at = pl.ds(k * BLOCK, BLOCK)
            value = conv(pv, taps_v, tp * channels, cols, PAD + k * BLOCK, BLOCK).astype(BF16)
            vals[at, cols] = value
            factor = dot(split(scale_in[:, k * BLOCK : (k + 1) * BLOCK]), expand2[:, lo:hi], ((0,), (0,)))
            scaled = (factor * value.astype(F32)).astype(BF16)
            state = dot(wrt[at, pl.ds(g * STATE, STATE)], scaled, ((0,), (0,)))
            if running is not None:
                inside[g][k] = running.astype(BF16)
                state = state + end_rows[k][:, lo:hi] * running
            running = state
        local_state[:, cols] = running
        for i in range(chunks_group):
            sending[g * chunks_group + i] = running[:, i * LANES : (i + 1) * LANES].astype(BF16)

        @pl.when(me == 0)
        def _(g=g):
            for i in range(chunks_group):
                chain(g * chunks_group + i).start()

    get_read.wait()
    pr[...] = dot(xs[...], wr[...])
    causal = (
        lax.broadcasted_iota(jnp.int32, (BLOCK, BLOCK), 0)
        >= lax.broadcasted_iota(jnp.int32, (BLOCK, BLOCK), 1)
    )
    owner = lax.broadcasted_iota(jnp.int32, (BLOCK, wide), 1) // HEAD
    for g in range(groups):
        lo, hi = g * wide, (g + 1) * wide
        cols = pl.ds(lo, wide)
        maps_at = pl.ds(g * STATE, STATE)
        for k in range(blocks):
            at = pl.ds(k * BLOCK, BLOCK)
            span = slice(k * BLOCK, (k + 1) * BLOCK)
            read = conv(pr, taps_r, tp * maps, maps_at, PAD + k * BLOCK, BLOCK).astype(BF16)
            rds[at, maps_at] = read
            scores = dot(read, wrt[at, maps_at], ((1,), (1,)))
            value = vals[at, cols]
            mixes, stacked = [], []
            for e in range(per_group):
                h = g * per_group + e
                gap = cum_cols[k][:, h : h + 1] - cums[k][h : h + 1]
                decay = jnp.exp(jnp.where(causal, gap, -jnp.inf))
                mixes.append((scores * decay * step[h : h + 1, span]).astype(BF16))
                stacked.append(jnp.where(owner == e, value, jnp.zeros_like(value)))
            y = dot(jnp.concatenate(mixes, axis=1), jnp.concatenate(stacked, axis=0))
            grown = dot(split(jnp.exp(cums[k])), expand2[:, lo:hi], ((0,), (0,)))
            if k > 0:
                y = y + grown * dot(read, inside[g][k])
            y_loc[at, cols] = y + skip_row[:, lo:hi] * value.astype(F32)
            fade[at, cols] = dot(split(jnp.exp(cums[k] + before[k])), expand2[:, lo:hi], ((0,), (0,)))
            pg[at, cols] = silu(pg[at, cols])

    base = PAD + rows
    new_value = jnp.concatenate(
        [conv(pv, taps_v, tp * channels, pl.ds(g * wide, wide), base, 1) for g in range(groups)], axis=1
    ).astype(BF16).astype(F32)
    new_write = [conv(pw, taps_w, tp * maps, pl.ds(g * STATE, STATE), base, 1).astype(BF16) for g in range(groups)]
    new_read = [conv(pr, taps_r, tp * maps, pl.ds(g * STATE, STATE), base, 1).astype(BF16) for g in range(groups)]
    new_gate = silu(pg[pl.ds(rows, 1)])
    new_decay_row = jnp.sum(expand * jnp.exp(-new_step * rates), axis=0, keepdims=True)
    new_step_row = jnp.sum(expand * new_step, axis=0, keepdims=True)

    @pl.when(me > 0)
    def _():
        for c in range(chunks):
            chain(c).wait_recv()
            at = pl.ds(c * LANES, LANES)
            state = received[c].astype(F32) * total_row[:, c * LANES : (c + 1) * LANES] + local_state[:, at]
            local_state[:, at] = state

            @pl.when(me < last)
            def _(c=c, state=state):
                sending[c] = state.astype(BF16)
                chain(c).start()

    def cache_copy(s):
        return pltpu.make_async_remote_copy(
            src_ref=cache.at[s], dst_ref=cache_out, send_sem=cache_send.at[s],
            recv_sem=cache_recv, device_id={"sp": s}, device_id_type=MESH,
        )

    def row_copy(s):
        return pltpu.make_async_remote_copy(
            src_ref=step_row, dst_ref=step_recv, send_sem=row_send.at[s],
            recv_sem=row_recv, device_id={"sp": s}, device_id_type=MESH,
        )

    own_cache = pltpu.make_async_copy(cache.at[last], cache_out, cache_recv)

    @pl.when(me == last)
    def _():
        for s in range(n):
            cache[s] = local_state[pl.ds(s * piece, piece)].astype(BF16)
        parts = []
        for g in range(groups):
            lo, hi = g * wide, (g + 1) * wide
            stored = local_state[:, pl.ds(lo, wide)].astype(BF16)
            read = jnp.broadcast_to(new_read[g], (PAD, STATE))
            fetched = dot(read, stored)[:1] * new_decay_row[:, lo:hi]
            overlap = jnp.sum(new_read[g].astype(F32) * new_write[g].astype(F32), axis=1, keepdims=True)
            value = new_value[:, lo:hi]
            mixed = fetched + new_step_row[:, lo:hi] * overlap * value + skip_row[:, lo:hi] * value
            gated = mixed * new_gate[:, lo:hi]
            mean = jnp.sum(gated * gated, axis=1, keepdims=True) * (1.0 / wide)
            parts.append(gated * lax.rsqrt(mean + EPSILON) * gain_row[:, lo:hi])
        row = jnp.broadcast_to(jnp.concatenate(parts, axis=1), (8, channels))
        step_row[...] = row
        step_recv[...] = row
        for s in range(last):
            cache_copy(s).start()
            row_copy(s).start()
        own_cache.start()

    def finish(k, g, arrived):
        at = pl.ds(k * BLOCK, BLOCK)
        cols = pl.ds(g * wide, wide)
        y = y_loc[at, cols]
        if arrived is not None:
            y = y + fade[at, cols] * dot(rds[at, pl.ds(g * STATE, STATE)], arrived)
        gated = y * pg[at, cols]
        mean = jnp.sum(gated * gated, axis=1, keepdims=True) * (1.0 / wide)
        normed = gated * lax.rsqrt(mean + EPSILON) * gain_row[:, g * wide : (g + 1) * wide]
        result[at, cols] = normed.astype(BF16)

    @pl.when(me == 0)
    def _():
        received[...] = jnp.zeros(received.shape, BF16)

    writes = []
    for g in range(groups):
        arrived = jnp.concatenate([received[g * chunks_group + i] for i in range(chunks_group)], axis=1)
        for k in range(blocks):
            finish(k, g, arrived)
    for k in range(blocks):
        at = pl.ds(k * BLOCK, BLOCK)
        copy = pltpu.make_async_copy(result.at[at], out.at[at], out_sem.at[k])
        copy.start()
        writes.append(copy)

    @pl.when(me < last)
    def _():
        for c in range(chunks):
            chain(c).wait_send()
        halo.wait_send()
        row_copy(0).wait_recv()
        cache_copy(0).wait_recv()

    columns = channels // n
    mine = lax.broadcasted_iota(jnp.int32, (8, channels), 1) % n == me
    picked = jnp.where(mine, step_recv[...], 0.0).astype(BF16)
    choose = (
        lax.broadcasted_iota(jnp.int32, (channels, columns), 0) // n
        == lax.broadcasted_iota(jnp.int32, (channels, columns), 1)
    ).astype(F32).astype(BF16)
    step_out[...] = dot(picked, choose)[:1].astype(BF16)

    @pl.when(me == last)
    def _():
        for s in range(last):
            cache_copy(s).wait_send()
            row_copy(s).wait_send()
        own_cache.wait()

    for copy in writes:
        copy.wait()


def on_device(
    tokens, fresh, w_value, w_write, w_read, w_gate, step_matrix, taps_v, taps_w, taps_r,
    log_rate, offset_bias, spike, bypass, gain,
):
    n = lax.axis_size("sp")
    rows, width = tokens.shape
    channels = w_value.shape[1]
    maps = w_write.shape[1]
    groups = maps // STATE
    chunks = channels // LANES
    blocks = rows // BLOCK
    piece = STATE // n
    any_space = pl.BlockSpec(memory_space=pl.ANY)
    vmem = pl.BlockSpec(memory_space=pltpu.VMEM)
    dma = pltpu.SemaphoreType.DMA
    out, cache, step = pl.pallas_call(
        functools.partial(kernel, n),
        out_shape=(
            jax.ShapeDtypeStruct((rows, channels), BF16),
            jax.ShapeDtypeStruct((piece, channels), BF16),
            jax.ShapeDtypeStruct((1, channels // n), BF16),
        ),
        in_specs=[any_space, vmem, any_space, any_space, any_space, any_space] + [vmem] * 9,
        out_specs=(any_space, any_space, vmem),
        scratch_shapes=[
            pltpu.VMEM((rows + 2 * PAD, width), BF16),
            pltpu.VMEM((width, channels), BF16),
            pltpu.VMEM((width, maps), BF16),
            pltpu.VMEM((width, maps), BF16),
            pltpu.VMEM((width, channels), BF16),
            pltpu.VMEM((rows + 2 * PAD, channels), F32),
            pltpu.VMEM((rows + 2 * PAD, maps), F32),
            pltpu.VMEM((rows + 2 * PAD, maps), F32),
            pltpu.VMEM((rows + PAD, channels), F32),
            pltpu.VMEM((step_matrix.shape[1], rows), F32),
            pltpu.VMEM((rows, channels), BF16),
            pltpu.VMEM((rows, maps), BF16),
            pltpu.VMEM((rows, maps), BF16),
            pltpu.VMEM((rows, channels), F32),
            pltpu.VMEM((rows, channels), F32),
            pltpu.VMEM((STATE, channels), F32),
            pltpu.VMEM((chunks, STATE, LANES), BF16),
            pltpu.VMEM((chunks, STATE, LANES), BF16),
            pltpu.VMEM((n, piece, channels), BF16),
            pltpu.VMEM((8, channels), F32),
            pltpu.VMEM((8, channels), F32),
            pltpu.VMEM((rows, channels), BF16),
            dma((3 + 2 * groups,)),
            dma, dma,
            dma((chunks,)), dma((chunks,)),
            dma((n,)), dma, dma((n,)), dma,
            dma((blocks,)),
        ],
        compiler_params=pltpu.CompilerParams(collective_id=0, has_side_effects=True),
    )(
        tokens, fresh.reshape(width // LANES, LANES), w_value, w_write, w_read, w_gate, step_matrix.T,
        taps_v, taps_w, taps_r, log_rate[None], offset_bias[None], spike.T, bypass[None],
        gain.reshape(-1, LANES),
    )
    return (out, cache, step.T)


def solution(mesh):
    placed = (
        P(("grp", "sp"), None), P("grp"), P(None, "tp"), P(None, "tp"), P(None, "tp"), P(None, "tp"),
        P(), P(), P(), P(), P(), P(), P(("grp", "sp"), "tp"), P(), P(),
    )
    return jax.shard_map(
        on_device,
        mesh=mesh,
        in_specs=placed,
        out_specs=(P(("grp", "sp"), "tp"), P(("grp", "sp"), "tp"), P(("grp", "tp"), "sp")),
        check_vma=False,
    )
```

```python
import functools

import jax
import jax.numpy as jnp
from jax import lax
from jax.experimental import pallas as pl
from jax.experimental.pallas import tpu as pltpu
from jax.sharding import PartitionSpec as P

HEAD = 64
STATE = 128
CONV = 4
BLOCK = 128
PAD = 16
LANES = 128
EPSILON = 1e-06
F32 = jnp.float32
BF16 = jnp.bfloat16
MESH = pl.DeviceIdType.MESH


def dot(a, b, dims=((1,), (0,)), precision=None):
    return lax.dot_general(a, b, (dims, ((), ())), precision=precision, preferred_element_type=F32)


def silu(x):
    half = 0.5 * x
    return half + half * jnp.tanh(half)


def softplus(x):
    return jnp.maximum(x, 0.0) + jnp.log1p(jnp.exp(-jnp.abs(x)))


def split(x):
    high = x.astype(BF16)
    return jnp.concatenate([high.astype(F32), x - high.astype(F32)], axis=0).astype(BF16)


def kernel(
    n, tokens, fresh_hbm, w_value, w_write, w_read, w_gate, step_hbm, taps_v_hbm, taps_w_hbm, taps_r_hbm,
    log_rate_hbm, bias_hbm, spike_hbm, bypass_hbm, gain_hbm,
    result, cache_in, step_out,
    fresh, step_t, taps_v, taps_w, taps_r, log_rate, offset_bias, spike_t, bypass, gain,
    xs, wv, ww, wr, wg, pv, pw, pr, pg, raw_t, vals, wrt, rds, y_loc, fade, local_state,
    received, sending, cache, step_row, step_recv,
    load_sem, halo_send, halo_recv, chain_send, chain_recv, cache_send, cache_recv,
    row_send, row_recv, small_sem,
):
    rows, width = tokens.shape
    channels = w_value.shape[1]
    maps = w_write.shape[1]
    groups = maps // STATE
    heads = channels // HEAD
    per_group = heads // groups
    wide = per_group * HEAD
    blocks = rows // BLOCK
    all_heads = step_t.shape[0]
    piece = STATE // n
    tp = lax.axis_index("tp")
    me = lax.axis_index("sp")
    last = n - 1
    chunks = channels // LANES
    chunks_group = wide // LANES

    loads = []

    def load(src, dst):
        copy = pltpu.make_async_copy(src, dst, load_sem.at[len(loads)])
        loads.append(copy)
        copy.start()
        return copy

    barrier = pltpu.get_barrier_semaphore()

    @pl.when(me > 0)
    def _():
        pl.semaphore_signal(barrier, inc=1, device_id={"sp": me - 1}, device_id_type=MESH)

    small = [
        pltpu.make_async_copy(src, dst, small_sem.at[i])
        for i, (src, dst) in enumerate((
            (fresh_hbm, fresh), (step_hbm, step_t), (taps_v_hbm, taps_v), (taps_w_hbm, taps_w),
            (taps_r_hbm, taps_r), (log_rate_hbm, log_rate), (bias_hbm, offset_bias),
            (spike_hbm, spike_t), (bypass_hbm, bypass), (gain_hbm, gain),
        ))
    ]
    get_tokens = load(tokens, xs.at[pl.ds(PAD, rows)])
    for copy in small:
        copy.start()
    get_gate = [load(w_gate.at[:, pl.ds(g * wide, wide)], wg.at[:, pl.ds(g * wide, wide)]) for g in range(groups)]
    get_write = load(w_write, ww)
    get_value = [load(w_value.at[:, pl.ds(g * wide, wide)], wv.at[:, pl.ds(g * wide, wide)]) for g in range(groups)]
    get_read = load(w_read, wr)

    @pl.when(me < last)
    def _():
        pl.semaphore_wait(barrier, 1)

    following = jnp.minimum(me + 1, last)
    halo = pltpu.make_async_remote_copy(
        src_ref=tokens.at[pl.ds(rows - PAD, PAD)], dst_ref=xs.at[pl.ds(0, PAD)],
        send_sem=halo_send, recv_sem=halo_recv, device_id={"sp": following}, device_id_type=MESH,
    )

    @pl.when(me < last)
    def _():
        halo.start()

    for copy in small:
        copy.wait()

    fresh_f = fresh[...].astype(F32)
    fresh_row = jnp.concatenate([fresh_f[i : i + 1] for i in range(width // LANES)], axis=1)
    xs[pl.ds(PAD + rows, PAD)] = jnp.broadcast_to(fresh_row, (PAD, width)).astype(BF16)

    @pl.when(me == 0)
    def _():
        xs[pl.ds(0, PAD)] = jnp.zeros((PAD, width), BF16)

    lane = lax.broadcasted_iota(jnp.int32, (heads, all_heads), 1)
    own = lane == lax.broadcasted_iota(jnp.int32, (heads, all_heads), 0) + tp * heads

    def column(ref):
        return jnp.sum(jnp.where(own, ref[...], 0.0), axis=1, keepdims=True)

    rates = jnp.exp(column(log_rate))
    bias = column(offset_bias)
    expand = (
        lax.broadcasted_iota(jnp.int32, (heads, channels), 1) // HEAD
        == lax.broadcasted_iota(jnp.int32, (heads, channels), 0)
    ).astype(F32)
    expand2 = jnp.concatenate([expand, expand], axis=0).astype(BF16)

    def spread(x):
        return dot(split(x), expand2, ((0,), (0,)))

    skip_row = jnp.sum(expand * column(bypass), axis=0, keepdims=True)
    gain_row = jnp.concatenate(
        [gain[pl.ds(tp * (channels // LANES) + i, 1)] for i in range(channels // LANES)], axis=1
    )

    get_tokens.wait()
    raw = dot(xs[pl.ds(PAD, rows + PAD)], step_t[...], ((1,), (1,)))
    raw_t[...] = raw[:rows].T
    if heads % 8 == 0:
        own_raw = raw_t[pl.ds(pl.multiple_of(tp * heads, 8), heads)]
    else:
        own_raw = dot(own.astype(F32), raw_t[...], precision=lax.Precision.HIGHEST)
    raw_new = jnp.sum(jnp.where(own, raw[rows : rows + 1], 0.0), axis=1, keepdims=True)
    step = softplus(own_raw + bias)
    new_step = softplus(raw_new + bias)
    log_decay = spike_t[...] - step * rates
    upper = (
        lax.broadcasted_iota(jnp.int32, (BLOCK, BLOCK), 0)
        <= lax.broadcasted_iota(jnp.int32, (BLOCK, BLOCK), 1)
    ).astype(F32)
    cums = [
        dot(log_decay[:, k * BLOCK : (k + 1) * BLOCK], upper, precision=lax.Precision.HIGHEST)
        for k in range(blocks)
    ]
    ends = [c[:, BLOCK - 1 :] for c in cums]
    before = [jnp.zeros_like(ends[0])]
    for k in range(blocks):
        before.append(before[k] + ends[k])
    scale_in = jnp.concatenate([jnp.exp(ends[k] - cums[k]) for k in range(blocks)], axis=1) * step
    cum_cols = [c.T for c in cums]
    end_rows = [jnp.sum(expand * jnp.exp(e), axis=0, keepdims=True) for e in ends]
    total_row = jnp.sum(expand * jnp.exp(before[blocks]), axis=0, keepdims=True)

    for g in range(groups):
        cols = pl.ds(g * wide, wide)
        get_gate[g].wait()
        pg[:, cols] = dot(xs[pl.ds(PAD, rows + PAD)], wg[:, cols])

    @pl.when(me > 0)
    def _():
        halo.wait_recv()

    def conv(src, taps, base, cols, start, count):
        own_cols = pl.ds(pl.multiple_of(base + cols.start, LANES), cols.size)
        weights = taps[:, own_cols].astype(F32)
        total = None
        for k in range(CONV):
            term = weights[k : k + 1] * src[pl.ds(start - (CONV - 1) + k, count), cols]
            total = term if total is None else total + term
        return silu(total)

    get_write.wait()
    pw[...] = dot(xs[...], ww[...])
    for g in range(groups):
        cols = pl.ds(g * STATE, STATE)
        for k in range(blocks):
            wrt[pl.ds(k * BLOCK, BLOCK), cols] = conv(pw, taps_w, tp * maps, cols, PAD + k * BLOCK, BLOCK).astype(BF16)

    def chain(c):
        return pltpu.make_async_remote_copy(
            src_ref=sending.at[c], dst_ref=received.at[c], send_sem=chain_send.at[c],
            recv_sem=chain_recv.at[c], device_id={"sp": following}, device_id_type=MESH,
        )

    inside = [[None] * blocks for _ in range(groups)]
    for g in range(groups):
        cols = pl.ds(g * wide, wide)
        get_value[g].wait()
        pv[:, cols] = dot(xs[...], wv[:, cols])
        lo, hi = g * wide, (g + 1) * wide
        running = None
        for k in range(blocks):
            at = pl.ds(k * BLOCK, BLOCK)
            value = conv(pv, taps_v, tp * channels, cols, PAD + k * BLOCK, BLOCK).astype(BF16)
            vals[at, cols] = value
            factor = dot(split(scale_in[:, k * BLOCK : (k + 1) * BLOCK]), expand2[:, lo:hi], ((0,), (0,)))
            scaled = (factor * value.astype(F32)).astype(BF16)
            state = dot(wrt[at, pl.ds(g * STATE, STATE)], scaled, ((0,), (0,)))
            if running is not None:
                inside[g][k] = running.astype(BF16)
                state = state + end_rows[k][:, lo:hi] * running
            running = state
        local_state[:, cols] = running
        for i in range(chunks_group):
            sending[g * chunks_group + i] = running[:, i * LANES : (i + 1) * LANES].astype(BF16)

        @pl.when(me == 0)
        def _(g=g):
            for i in range(chunks_group):
                chain(g * chunks_group + i).start()

    get_read.wait()
    pr[...] = dot(xs[...], wr[...])
    causal = (
        lax.broadcasted_iota(jnp.int32, (BLOCK, BLOCK), 0)
        >= lax.broadcasted_iota(jnp.int32, (BLOCK, BLOCK), 1)
    )
    owner = lax.broadcasted_iota(jnp.int32, (BLOCK, wide), 1) // HEAD
    for g in range(groups):
        lo, hi = g * wide, (g + 1) * wide
        cols = pl.ds(lo, wide)
        maps_at = pl.ds(g * STATE, STATE)
        for k in range(blocks):
            at = pl.ds(k * BLOCK, BLOCK)
            span = slice(k * BLOCK, (k + 1) * BLOCK)
            read = conv(pr, taps_r, tp * maps, maps_at, PAD + k * BLOCK, BLOCK).astype(BF16)
            rds[at, maps_at] = read
            scores = dot(read, wrt[at, maps_at], ((1,), (1,)))
            value = vals[at, cols]
            mixes, stacked = [], []
            for e in range(per_group):
                h = g * per_group + e
                gap = cum_cols[k][:, h : h + 1] - cums[k][h : h + 1]
                decay = jnp.exp(jnp.where(causal, gap, -jnp.inf))
                mixes.append((scores * decay * step[h : h + 1, span]).astype(BF16))
                stacked.append(jnp.where(owner == e, value, jnp.zeros_like(value)))
            y = dot(jnp.concatenate(mixes, axis=1), jnp.concatenate(stacked, axis=0))
            grown = dot(split(jnp.exp(cums[k])), expand2[:, lo:hi], ((0,), (0,)))
            if k > 0:
                y = y + grown * dot(read, inside[g][k])
            y_loc[at, cols] = y + skip_row[:, lo:hi] * value.astype(F32)
            fade[at, cols] = dot(split(jnp.exp(cums[k] + before[k])), expand2[:, lo:hi], ((0,), (0,)))
            pg[at, cols] = silu(pg[at, cols])

    base = PAD + rows
    new_value = jnp.concatenate(
        [conv(pv, taps_v, tp * channels, pl.ds(g * wide, wide), base, 1) for g in range(groups)], axis=1
    ).astype(BF16).astype(F32)
    new_write = [conv(pw, taps_w, tp * maps, pl.ds(g * STATE, STATE), base, 1).astype(BF16) for g in range(groups)]
    new_read = [conv(pr, taps_r, tp * maps, pl.ds(g * STATE, STATE), base, 1).astype(BF16) for g in range(groups)]
    new_gate = silu(pg[pl.ds(rows, 1)])
    new_decay_row = jnp.sum(expand * jnp.exp(-new_step * rates), axis=0, keepdims=True)
    new_step_row = jnp.sum(expand * new_step, axis=0, keepdims=True)

    def cache_copy(s, c):
        return pltpu.make_async_remote_copy(
            src_ref=cache.at[c, s], dst_ref=cache_in.at[c], send_sem=cache_send.at[c, s],
            recv_sem=cache_recv.at[c], device_id={"sp": s}, device_id_type=MESH,
        )

    def row_copy(s):
        return pltpu.make_async_remote_copy(
            src_ref=step_row, dst_ref=step_recv, send_sem=row_send.at[s],
            recv_sem=row_recv, device_id={"sp": s}, device_id_type=MESH,
        )

    @pl.when(me > 0)
    def _():
        for c in range(chunks):
            chain(c).wait_recv()
            at = pl.ds(c * LANES, LANES)
            state = received[c].astype(F32) * total_row[:, c * LANES : (c + 1) * LANES] + local_state[:, at]

            @pl.when(me < last)
            def _(c=c, state=state):
                sending[c] = state.astype(BF16)
                chain(c).start()

            @pl.when(me == last)
            def _(c=c, state=state, at=at):
                local_state[:, at] = state
                for s in range(n):
                    cache[c, s] = state[s * piece : (s + 1) * piece].astype(BF16)
                cache_in[c] = state[last * piece :].astype(BF16)
                for s in range(last):
                    cache_copy(s, c).start()

    @pl.when(me == last)
    def _():
        parts = []
        for g in range(groups):
            lo, hi = g * wide, (g + 1) * wide
            stored = local_state[:, pl.ds(lo, wide)].astype(BF16)
            read = jnp.broadcast_to(new_read[g], (PAD, STATE))
            fetched = dot(read, stored)[:1] * new_decay_row[:, lo:hi]
            overlap = jnp.sum(new_read[g].astype(F32) * new_write[g].astype(F32), axis=1, keepdims=True)
            value = new_value[:, lo:hi]
            mixed = fetched + new_step_row[:, lo:hi] * overlap * value + skip_row[:, lo:hi] * value
            gated = mixed * new_gate[:, lo:hi]
            mean = jnp.sum(gated * gated, axis=1, keepdims=True) * (1.0 / wide)
            parts.append(gated * lax.rsqrt(mean + EPSILON) * gain_row[:, lo:hi])
        for c in range(chunks):
            row = parts[c // chunks_group][:, (c % chunks_group) * LANES : (c % chunks_group + 1) * LANES]
            step_row[pl.ds(c, 1)] = row
            step_recv[pl.ds(c, 1)] = row
        for s in range(last):
            row_copy(s).start()

    def finish(k, g, arrived):
        at = pl.ds(k * BLOCK, BLOCK)
        cols = pl.ds(g * wide, wide)
        y = y_loc[at, cols]
        if arrived is not None:
            y = y + fade[at, cols] * dot(rds[at, pl.ds(g * STATE, STATE)], arrived)
        gated = y * pg[at, cols]
        mean = jnp.sum(gated * gated, axis=1, keepdims=True) * (1.0 / wide)
        normed = gated * lax.rsqrt(mean + EPSILON) * gain_row[:, g * wide : (g + 1) * wide]
        result[at, cols] = normed.astype(BF16)

    @pl.when(me == 0)
    def _():
        received[...] = jnp.zeros(received.shape, BF16)

    for g in range(groups):
        arrived = jnp.concatenate([received[g * chunks_group + i] for i in range(chunks_group)], axis=1)
        for k in range(blocks):
            finish(k, g, arrived)

    @pl.when(me < last)
    def _():
        for c in range(chunks):
            chain(c).wait_send()
        halo.wait_send()
        row_copy(0).wait_recv()
        for c in range(chunks):
            cache_copy(0, c).wait_recv()

    columns = channels // n
    mine = lax.broadcasted_iota(jnp.int32, (8, channels), 1) % n == me
    whole = jnp.concatenate([step_recv[pl.ds(c, 1)] for c in range(chunks)], axis=1)
    picked = jnp.where(mine, jnp.broadcast_to(whole, (8, channels)), 0.0).astype(BF16)
    choose = (
        lax.broadcasted_iota(jnp.int32, (channels, columns), 0) // n
        == lax.broadcasted_iota(jnp.int32, (channels, columns), 1)
    ).astype(F32).astype(BF16)
    step_out[...] = dot(picked, choose)[:1].astype(BF16)

    @pl.when(me == last)
    def _():
        for s in range(last):
            row_copy(s).wait_send()
            for c in range(chunks):
                cache_copy(s, c).wait_send()


def deliver(result, cache_in, step, out, cache_out, step_out, sems):
    copies = [
        pltpu.make_async_copy(result, out, sems.at[0]),
        pltpu.make_async_copy(step, step_out, sems.at[1]),
    ]
    for c in range(cache_in.shape[0]):
        copies.append(pltpu.make_async_copy(cache_in.at[c], cache_out.at[:, pl.ds(c * LANES, LANES)], sems.at[2 + c]))
    for copy in copies:
        copy.start()
    for copy in copies:
        copy.wait()


def on_device(
    tokens, fresh, w_value, w_write, w_read, w_gate, step_matrix, taps_v, taps_w, taps_r,
    log_rate, offset_bias, spike, bypass, gain,
):
    n = lax.axis_size("sp")
    rows, width = tokens.shape
    channels = w_value.shape[1]
    maps = w_write.shape[1]
    groups = maps // STATE
    chunks = channels // LANES
    piece = STATE // n
    any_space = pl.BlockSpec(memory_space=pl.ANY)
    vmem = pl.BlockSpec(memory_space=pltpu.VMEM)
    dma = pltpu.SemaphoreType.DMA
    heads = channels // HEAD
    all_heads = step_matrix.shape[1]
    passed = pl.pallas_call(
        functools.partial(kernel, n),
        out_shape=(
            pltpu.VMEM((rows, channels), BF16),
            pltpu.VMEM((chunks, piece, LANES), BF16),
            pltpu.VMEM((1, channels // n), BF16),
        ),
        in_specs=[any_space] * 15,
        out_specs=(vmem, vmem, vmem),
        scratch_shapes=[
            pltpu.VMEM((width // LANES, LANES), BF16),
            pltpu.VMEM((all_heads, width), BF16),
            pltpu.VMEM(taps_v.shape, BF16),
            pltpu.VMEM(taps_w.shape, BF16),
            pltpu.VMEM(taps_r.shape, BF16),
            pltpu.VMEM((1, all_heads), F32),
            pltpu.VMEM((1, all_heads), F32),
            pltpu.VMEM((heads, rows), F32),
            pltpu.VMEM((1, all_heads), F32),
            pltpu.VMEM((gain.shape[0] // LANES, LANES), F32),
            pltpu.VMEM((rows + 2 * PAD, width), BF16),
            pltpu.VMEM((width, channels), BF16),
            pltpu.VMEM((width, maps), BF16),
            pltpu.VMEM((width, maps), BF16),
            pltpu.VMEM((width, channels), BF16),
            pltpu.VMEM((rows + 2 * PAD, channels), F32),
            pltpu.VMEM((rows + 2 * PAD, maps), F32),
            pltpu.VMEM((rows + 2 * PAD, maps), F32),
            pltpu.VMEM((rows + PAD, channels), F32),
            pltpu.VMEM((step_matrix.shape[1], rows), F32),
            pltpu.VMEM((rows, channels), BF16),
            pltpu.VMEM((rows, maps), BF16),
            pltpu.VMEM((rows, maps), BF16),
            pltpu.VMEM((rows, channels), F32),
            pltpu.VMEM((rows, channels), F32),
            pltpu.VMEM((STATE, channels), F32),
            pltpu.VMEM((chunks, STATE, LANES), BF16),
            pltpu.VMEM((chunks, STATE, LANES), BF16),
            pltpu.VMEM((chunks, n, piece, LANES), BF16),
            pltpu.VMEM((8, LANES), F32),
            pltpu.VMEM((8, LANES), F32),
            dma((3 + 2 * groups,)),
            dma, dma,
            dma((chunks,)), dma((chunks,)),
            dma((chunks, n)), dma((chunks,)), dma((n,)), dma,
            dma((10,)),
        ],
        compiler_params=pltpu.CompilerParams(collective_id=0, has_side_effects=True),
    )(
        tokens, fresh.reshape(width // LANES, LANES), w_value, w_write, w_read, w_gate, step_matrix.T,
        taps_v, taps_w, taps_r, log_rate[None], offset_bias[None], spike.T, bypass[None],
        gain.reshape(-1, LANES),
    )
    out, cache, step = pl.pallas_call(
        deliver,
        out_shape=(
            jax.ShapeDtypeStruct((rows, channels), BF16),
            jax.ShapeDtypeStruct((piece, channels), BF16),
            jax.ShapeDtypeStruct((1, channels // n), BF16),
        ),
        in_specs=[vmem] * 3,
        out_specs=(any_space,) * 3,
        scratch_shapes=[dma((2 + chunks,))],
    )(*(pltpu.with_memory_space_constraint(x, pltpu.VMEM) for x in passed))
    return (out, cache, step.T)


def solution(mesh):
    placed = (
        P(("grp", "sp"), None), P("grp"), P(None, "tp"), P(None, "tp"), P(None, "tp"), P(None, "tp"),
        P(), P(), P(), P(), P(), P(), P(("grp", "sp"), "tp"), P(), P(),
    )
    return jax.shard_map(
        on_device,
        mesh=mesh,
        in_specs=placed,
        out_specs=(P(("grp", "sp"), "tp"), P(("grp", "sp"), "tp"), P(("grp", "tp"), "sp")),
        check_vma=False,
    )
```

```python
import functools

import jax
import jax.numpy as jnp
from jax import lax
from jax.experimental import pallas as pl
from jax.experimental.pallas import tpu as pltpu
from jax.sharding import PartitionSpec as P

HEAD = 64
STATE = 128
CONV = 4
BLOCK = 128
PAD = 16
LANES = 128
CUTS = 2
EPSILON = 1e-06
F32 = jnp.float32
BF16 = jnp.bfloat16
MESH = pl.DeviceIdType.MESH


def dot(a, b, dims=((1,), (0,)), precision=None):
    return lax.dot_general(a, b, (dims, ((), ())), precision=precision, preferred_element_type=F32)


def silu(x):
    half = 0.5 * x
    return half + half * jnp.tanh(half)


def softplus(x):
    return jnp.maximum(x, 0.0) + jnp.log1p(jnp.exp(-jnp.abs(x)))


def split(x):
    high = x.astype(BF16)
    return jnp.concatenate([high.astype(F32), x - high.astype(F32)], axis=0).astype(BF16)


def kernel(
    n, tokens, fresh_hbm, w_value, w_write, w_read, w_gate, step_hbm, taps_v_hbm, taps_w_hbm, taps_r_hbm,
    log_rate_hbm, bias_hbm, spike_hbm, bypass_hbm, gain_hbm,
    result, cache_in, step_out,
    fresh, step_t, taps_v, taps_w, taps_r, log_rate, offset_bias, spike_t, bypass, gain,
    xs, wv, ww, wr, wg, pv, pw, pr, pg, raw_t, vals, wrt, rds, y_loc, fade, local_state,
    received, sending, cache, step_row, step_recv,
    load_sem, halo_send, halo_recv, chain_send, chain_recv, cache_send, cache_recv,
    row_send, row_recv, small_sem,
):
    rows, width = tokens.shape
    channels = w_value.shape[1]
    maps = w_write.shape[1]
    groups = maps // STATE
    heads = channels // HEAD
    per_group = heads // groups
    wide = per_group * HEAD
    blocks = rows // BLOCK
    all_heads = step_t.shape[0]
    piece = STATE // n
    tp = lax.axis_index("tp")
    me = lax.axis_index("sp")
    last = n - 1
    chunks = channels // LANES
    chunks_group = wide // LANES

    loads = []

    def load(src, dst):
        copy = pltpu.make_async_copy(src, dst, load_sem.at[len(loads)])
        loads.append(copy)
        copy.start()
        return copy

    barrier = pltpu.get_barrier_semaphore()

    @pl.when(me > 0)
    def _():
        pl.semaphore_signal(barrier, inc=1, device_id={"sp": me - 1}, device_id_type=MESH)

    small = [
        pltpu.make_async_copy(src, dst, small_sem.at[i])
        for i, (src, dst) in enumerate((
            (fresh_hbm, fresh), (step_hbm, step_t), (taps_v_hbm, taps_v), (taps_w_hbm, taps_w),
            (taps_r_hbm, taps_r), (log_rate_hbm, log_rate), (bias_hbm, offset_bias),
            (spike_hbm, spike_t), (bypass_hbm, bypass), (gain_hbm, gain),
        ))
    ]
    get_tokens = load(tokens, xs.at[pl.ds(PAD, rows)])
    for copy in small:
        copy.start()
    get_gate = [load(w_gate.at[:, pl.ds(g * wide, wide)], wg.at[:, pl.ds(g * wide, wide)]) for g in range(groups)]
    get_write = load(w_write, ww)
    get_value = [load(w_value.at[:, pl.ds(g * wide, wide)], wv.at[:, pl.ds(g * wide, wide)]) for g in range(groups)]
    get_read = load(w_read, wr)

    @pl.when(me < last)
    def _():
        pl.semaphore_wait(barrier, 1)

    following = jnp.minimum(me + 1, last)
    halo = pltpu.make_async_remote_copy(
        src_ref=tokens.at[pl.ds(rows - PAD, PAD)], dst_ref=xs.at[pl.ds(0, PAD)],
        send_sem=halo_send, recv_sem=halo_recv, device_id={"sp": following}, device_id_type=MESH,
    )

    @pl.when(me < last)
    def _():
        halo.start()

    for copy in small:
        copy.wait()

    fresh_f = fresh[...].astype(F32)
    fresh_row = jnp.concatenate([fresh_f[i : i + 1] for i in range(width // LANES)], axis=1)
    xs[pl.ds(PAD + rows, PAD)] = jnp.broadcast_to(fresh_row, (PAD, width)).astype(BF16)

    @pl.when(me == 0)
    def _():
        xs[pl.ds(0, PAD)] = jnp.zeros((PAD, width), BF16)

    lane = lax.broadcasted_iota(jnp.int32, (heads, all_heads), 1)
    own = lane == lax.broadcasted_iota(jnp.int32, (heads, all_heads), 0) + tp * heads

    def column(ref):
        return jnp.sum(jnp.where(own, ref[...], 0.0), axis=1, keepdims=True)

    rates = jnp.exp(column(log_rate))
    bias = column(offset_bias)
    expand = (
        lax.broadcasted_iota(jnp.int32, (heads, channels), 1) // HEAD
        == lax.broadcasted_iota(jnp.int32, (heads, channels), 0)
    ).astype(F32)
    expand2 = jnp.concatenate([expand, expand], axis=0).astype(BF16)

    def spread(x):
        return dot(split(x), expand2, ((0,), (0,)))

    skip_row = jnp.sum(expand * column(bypass), axis=0, keepdims=True)
    gain_row = jnp.concatenate(
        [gain[pl.ds(tp * (channels // LANES) + i, 1)] for i in range(channels // LANES)], axis=1
    )

    get_tokens.wait()
    raw = dot(xs[pl.ds(PAD, rows + PAD)], step_t[...], ((1,), (1,)))
    raw_t[...] = raw[:rows].T
    if heads % 8 == 0:
        own_raw = raw_t[pl.ds(pl.multiple_of(tp * heads, 8), heads)]
    else:
        own_raw = dot(own.astype(F32), raw_t[...], precision=lax.Precision.HIGHEST)
    raw_new = jnp.sum(jnp.where(own, raw[rows : rows + 1], 0.0), axis=1, keepdims=True)
    step = softplus(own_raw + bias)
    new_step = softplus(raw_new + bias)
    log_decay = spike_t[...] - step * rates
    upper = (
        lax.broadcasted_iota(jnp.int32, (BLOCK, BLOCK), 0)
        <= lax.broadcasted_iota(jnp.int32, (BLOCK, BLOCK), 1)
    ).astype(F32)
    cums = [
        dot(log_decay[:, k * BLOCK : (k + 1) * BLOCK], upper, precision=lax.Precision.HIGHEST)
        for k in range(blocks)
    ]
    ends = [c[:, BLOCK - 1 :] for c in cums]
    before = [jnp.zeros_like(ends[0])]
    for k in range(blocks):
        before.append(before[k] + ends[k])
    scale_in = jnp.concatenate([jnp.exp(ends[k] - cums[k]) for k in range(blocks)], axis=1) * step
    cum_cols = [c.T for c in cums]
    end_rows = [jnp.sum(expand * jnp.exp(e), axis=0, keepdims=True) for e in ends]
    total_row = jnp.sum(expand * jnp.exp(before[blocks]), axis=0, keepdims=True)

    @pl.when(me > 0)
    def _():
        halo.wait_recv()

    def conv(src, taps, base, cols, start, count):
        own_cols = pl.ds(pl.multiple_of(base + cols.start, LANES), cols.size)
        weights = taps[:, own_cols].astype(F32)
        total = None
        for k in range(CONV):
            term = weights[k : k + 1] * src[pl.ds(start - (CONV - 1) + k, count), cols]
            total = term if total is None else total + term
        return silu(total)

    get_write.wait()
    pw[...] = dot(xs[...], ww[...])
    for g in range(groups):
        cols = pl.ds(g * STATE, STATE)
        for k in range(blocks):
            wrt[pl.ds(k * BLOCK, BLOCK), cols] = conv(pw, taps_w, tp * maps, cols, PAD + k * BLOCK, BLOCK).astype(BF16)

    def chain(c, part):
        at = pl.ds(part * (STATE // CUTS), STATE // CUTS)
        return pltpu.make_async_remote_copy(
            src_ref=sending.at[c, at], dst_ref=received.at[c, at], send_sem=chain_send.at[c, part],
            recv_sem=chain_recv.at[c, part], device_id={"sp": following}, device_id_type=MESH,
        )

    inside = [[None] * blocks for _ in range(groups)]
    for g in range(groups):
        cols = pl.ds(g * wide, wide)
        get_value[g].wait()
        pv[:, cols] = dot(xs[...], wv[:, cols])
        lo, hi = g * wide, (g + 1) * wide
        running = None
        for k in range(blocks):
            at = pl.ds(k * BLOCK, BLOCK)
            value = conv(pv, taps_v, tp * channels, cols, PAD + k * BLOCK, BLOCK).astype(BF16)
            vals[at, cols] = value
            factor = dot(split(scale_in[:, k * BLOCK : (k + 1) * BLOCK]), expand2[:, lo:hi], ((0,), (0,)))
            scaled = (factor * value.astype(F32)).astype(BF16)
            state = dot(wrt[at, pl.ds(g * STATE, STATE)], scaled, ((0,), (0,)))
            if running is not None:
                inside[g][k] = running.astype(BF16)
                state = state + end_rows[k][:, lo:hi] * running
            running = state
        local_state[:, cols] = running
        for i in range(chunks_group):
            sending[g * chunks_group + i] = running[:, i * LANES : (i + 1) * LANES].astype(BF16)

        @pl.when(me == 0)
        def _(g=g):
            for i in range(chunks_group):
                for part in range(CUTS):
                    chain(g * chunks_group + i, part).start()

    for g in range(groups):
        cols = pl.ds(g * wide, wide)
        get_gate[g].wait()
        pg[:, cols] = dot(xs[pl.ds(PAD, rows + PAD)], wg[:, cols])

    get_read.wait()
    pr[...] = dot(xs[...], wr[...])
    causal = (
        lax.broadcasted_iota(jnp.int32, (BLOCK, BLOCK), 0)
        >= lax.broadcasted_iota(jnp.int32, (BLOCK, BLOCK), 1)
    )
    owner = lax.broadcasted_iota(jnp.int32, (BLOCK, wide), 1) // HEAD
    for g in range(groups):
        lo, hi = g * wide, (g + 1) * wide
        cols = pl.ds(lo, wide)
        maps_at = pl.ds(g * STATE, STATE)
        for k in range(blocks):
            at = pl.ds(k * BLOCK, BLOCK)
            span = slice(k * BLOCK, (k + 1) * BLOCK)
            read = conv(pr, taps_r, tp * maps, maps_at, PAD + k * BLOCK, BLOCK).astype(BF16)
            rds[at, maps_at] = read
            scores = dot(read, wrt[at, maps_at], ((1,), (1,)))
            value = vals[at, cols]
            mixes, stacked = [], []
            for e in range(per_group):
                h = g * per_group + e
                gap = cum_cols[k][:, h : h + 1] - cums[k][h : h + 1]
                decay = jnp.exp(jnp.where(causal, gap, -jnp.inf))
                mixes.append((scores * decay * step[h : h + 1, span]).astype(BF16))
                stacked.append(jnp.where(owner == e, value, jnp.zeros_like(value)))
            y = dot(jnp.concatenate(mixes, axis=1), jnp.concatenate(stacked, axis=0))
            grown = dot(split(jnp.exp(cums[k])), expand2[:, lo:hi], ((0,), (0,)))
            if k > 0:
                y = y + grown * dot(read, inside[g][k])
            y_loc[at, cols] = y + skip_row[:, lo:hi] * value.astype(F32)
            fade[at, cols] = dot(split(jnp.exp(cums[k] + before[k])), expand2[:, lo:hi], ((0,), (0,)))
            pg[at, cols] = silu(pg[at, cols])

    base = PAD + rows
    new_value = jnp.concatenate(
        [conv(pv, taps_v, tp * channels, pl.ds(g * wide, wide), base, 1) for g in range(groups)], axis=1
    ).astype(BF16).astype(F32)
    new_write = [conv(pw, taps_w, tp * maps, pl.ds(g * STATE, STATE), base, 1).astype(BF16) for g in range(groups)]
    new_read = [conv(pr, taps_r, tp * maps, pl.ds(g * STATE, STATE), base, 1).astype(BF16) for g in range(groups)]
    new_gate = silu(pg[pl.ds(rows, 1)])
    new_decay_row = jnp.sum(expand * jnp.exp(-new_step * rates), axis=0, keepdims=True)
    new_step_row = jnp.sum(expand * new_step, axis=0, keepdims=True)

    def cache_copy(s, c):
        return pltpu.make_async_remote_copy(
            src_ref=cache.at[c, s], dst_ref=cache_in.at[c], send_sem=cache_send.at[c, s],
            recv_sem=cache_recv.at[c], device_id={"sp": s}, device_id_type=MESH,
        )

    def row_copy(s):
        return pltpu.make_async_remote_copy(
            src_ref=step_row, dst_ref=step_recv, send_sem=row_send.at[s],
            recv_sem=row_recv, device_id={"sp": s}, device_id_type=MESH,
        )

    @pl.when(me > 0)
    def _():
        for c in range(chunks):
            at = pl.ds(c * LANES, LANES)
            for part in range(CUTS):
                chain(c, part).wait_recv()
                span = pl.ds(part * (STATE // CUTS), STATE // CUTS)
                local_state[span, at] = (
                    received[c, span].astype(F32) * total_row[:, c * LANES : (c + 1) * LANES] + local_state[span, at]
                )

                @pl.when(me < last)
                def _(c=c, part=part, span=span, at=at):
                    sending[c, span] = local_state[span, at].astype(BF16)
                    chain(c, part).start()

            @pl.when(me == last)
            def _(c=c, at=at):
                state = local_state[:, at]
                for s in range(n):
                    cache[c, s] = state[s * piece : (s + 1) * piece].astype(BF16)
                cache_in[c] = state[last * piece :].astype(BF16)
                for s in range(last):
                    cache_copy(s, c).start()

    @pl.when(me == last)
    def _():
        parts = []
        for g in range(groups):
            lo, hi = g * wide, (g + 1) * wide
            stored = local_state[:, pl.ds(lo, wide)].astype(BF16)
            read = jnp.broadcast_to(new_read[g], (PAD, STATE))
            fetched = dot(read, stored)[:1] * new_decay_row[:, lo:hi]
            overlap = jnp.sum(new_read[g].astype(F32) * new_write[g].astype(F32), axis=1, keepdims=True)
            value = new_value[:, lo:hi]
            mixed = fetched + new_step_row[:, lo:hi] * overlap * value + skip_row[:, lo:hi] * value
            gated = mixed * new_gate[:, lo:hi]
            mean = jnp.sum(gated * gated, axis=1, keepdims=True) * (1.0 / wide)
            parts.append(gated * lax.rsqrt(mean + EPSILON) * gain_row[:, lo:hi])
        for c in range(chunks):
            row = parts[c // chunks_group][:, (c % chunks_group) * LANES : (c % chunks_group + 1) * LANES]
            step_row[pl.ds(c, 1)] = row
            step_recv[pl.ds(c, 1)] = row
        for s in range(last):
            row_copy(s).start()

    def finish(k, g, arrived):
        at = pl.ds(k * BLOCK, BLOCK)
        cols = pl.ds(g * wide, wide)
        y = y_loc[at, cols]
        if arrived is not None:
            y = y + fade[at, cols] * dot(rds[at, pl.ds(g * STATE, STATE)], arrived)
        gated = y * pg[at, cols]
        mean = jnp.sum(gated * gated, axis=1, keepdims=True) * (1.0 / wide)
        normed = gated * lax.rsqrt(mean + EPSILON) * gain_row[:, g * wide : (g + 1) * wide]
        result[at, cols] = normed.astype(BF16)

    @pl.when(me == 0)
    def _():
        received[...] = jnp.zeros(received.shape, BF16)

    for g in range(groups):
        arrived = jnp.concatenate([received[g * chunks_group + i] for i in range(chunks_group)], axis=1)
        for k in range(blocks):
            finish(k, g, arrived)

    @pl.when(me < last)
    def _():
        for c in range(chunks):
            for part in range(CUTS):
                chain(c, part).wait_send()
        halo.wait_send()
        row_copy(0).wait_recv()
        for c in range(chunks):
            cache_copy(0, c).wait_recv()

    columns = channels // n
    mine = lax.broadcasted_iota(jnp.int32, (8, channels), 1) % n == me
    whole = jnp.concatenate([step_recv[pl.ds(c, 1)] for c in range(chunks)], axis=1)
    picked = jnp.where(mine, jnp.broadcast_to(whole, (8, channels)), 0.0).astype(BF16)
    choose = (
        lax.broadcasted_iota(jnp.int32, (channels, columns), 0) // n
        == lax.broadcasted_iota(jnp.int32, (channels, columns), 1)
    ).astype(F32).astype(BF16)
    step_out[...] = dot(picked, choose)[:1].astype(BF16)

    @pl.when(me == last)
    def _():
        for s in range(last):
            row_copy(s).wait_send()
            for c in range(chunks):
                cache_copy(s, c).wait_send()


def deliver(result, cache_in, step, out, cache_out, step_out, sems):
    copies = [
        pltpu.make_async_copy(result, out, sems.at[0]),
        pltpu.make_async_copy(step, step_out, sems.at[1]),
    ]
    for c in range(cache_in.shape[0]):
        copies.append(pltpu.make_async_copy(cache_in.at[c], cache_out.at[:, pl.ds(c * LANES, LANES)], sems.at[2 + c]))
    for copy in copies:
        copy.start()
    for copy in copies:
        copy.wait()


def on_device(
    tokens, fresh, w_value, w_write, w_read, w_gate, step_matrix, taps_v, taps_w, taps_r,
    log_rate, offset_bias, spike, bypass, gain,
):
    n = lax.axis_size("sp")
    rows, width = tokens.shape
    channels = w_value.shape[1]
    maps = w_write.shape[1]
    groups = maps // STATE
    chunks = channels // LANES
    piece = STATE // n
    any_space = pl.BlockSpec(memory_space=pl.ANY)
    vmem = pl.BlockSpec(memory_space=pltpu.VMEM)
    dma = pltpu.SemaphoreType.DMA
    heads = channels // HEAD
    all_heads = step_matrix.shape[1]
    passed = pl.pallas_call(
        functools.partial(kernel, n),
        out_shape=(
            pltpu.VMEM((rows, channels), BF16),
            pltpu.VMEM((chunks, piece, LANES), BF16),
            pltpu.VMEM((1, channels // n), BF16),
        ),
        in_specs=[any_space] * 15,
        out_specs=(vmem, vmem, vmem),
        scratch_shapes=[
            pltpu.VMEM((width // LANES, LANES), BF16),
            pltpu.VMEM((all_heads, width), BF16),
            pltpu.VMEM(taps_v.shape, BF16),
            pltpu.VMEM(taps_w.shape, BF16),
            pltpu.VMEM(taps_r.shape, BF16),
            pltpu.VMEM((1, all_heads), F32),
            pltpu.VMEM((1, all_heads), F32),
            pltpu.VMEM((heads, rows), F32),
            pltpu.VMEM((1, all_heads), F32),
            pltpu.VMEM((gain.shape[0] // LANES, LANES), F32),
            pltpu.VMEM((rows + 2 * PAD, width), BF16),
            pltpu.VMEM((width, channels), BF16),
            pltpu.VMEM((width, maps), BF16),
            pltpu.VMEM((width, maps), BF16),
            pltpu.VMEM((width, channels), BF16),
            pltpu.VMEM((rows + 2 * PAD, channels), F32),
            pltpu.VMEM((rows + 2 * PAD, maps), F32),
            pltpu.VMEM((rows + 2 * PAD, maps), F32),
            pltpu.VMEM((rows + PAD, channels), F32),
            pltpu.VMEM((step_matrix.shape[1], rows), F32),
            pltpu.VMEM((rows, channels), BF16),
            pltpu.VMEM((rows, maps), BF16),
            pltpu.VMEM((rows, maps), BF16),
            pltpu.VMEM((rows, channels), F32),
            pltpu.VMEM((rows, channels), F32),
            pltpu.VMEM((STATE, channels), F32),
            pltpu.VMEM((chunks, STATE, LANES), BF16),
            pltpu.VMEM((chunks, STATE, LANES), BF16),
            pltpu.VMEM((chunks, n, piece, LANES), BF16),
            pltpu.VMEM((8, LANES), F32),
            pltpu.VMEM((8, LANES), F32),
            dma((3 + 2 * groups,)),
            dma, dma,
            dma((chunks, CUTS)), dma((chunks, CUTS)),
            dma((chunks, n)), dma((chunks,)), dma((n,)), dma,
            dma((10,)),
        ],
        compiler_params=pltpu.CompilerParams(collective_id=0, has_side_effects=True),
    )(
        tokens, fresh.reshape(width // LANES, LANES), w_value, w_write, w_read, w_gate, step_matrix.T,
        taps_v, taps_w, taps_r, log_rate[None], offset_bias[None], spike.T, bypass[None],
        gain.reshape(-1, LANES),
    )
    out, cache, step = pl.pallas_call(
        deliver,
        out_shape=(
            jax.ShapeDtypeStruct((rows, channels), BF16),
            jax.ShapeDtypeStruct((piece, channels), BF16),
            jax.ShapeDtypeStruct((1, channels // n), BF16),
        ),
        in_specs=[vmem] * 3,
        out_specs=(any_space,) * 3,
        scratch_shapes=[dma((2 + chunks,))],
    )(*(pltpu.with_memory_space_constraint(x, pltpu.VMEM) for x in passed))
    return (out, cache, step.T)


def solution(mesh):
    placed = (
        P(("grp", "sp"), None), P("grp"), P(None, "tp"), P(None, "tp"), P(None, "tp"), P(None, "tp"),
        P(), P(), P(), P(), P(), P(), P(("grp", "sp"), "tp"), P(), P(),
    )
    return jax.shard_map(
        on_device,
        mesh=mesh,
        in_specs=placed,
        out_specs=(P(("grp", "sp"), "tp"), P(("grp", "sp"), "tp"), P(("grp", "tp"), "sp")),
        check_vma=False,
    )
```
